32 devices in a mesh: ep: 8 (over z, y), tp: 4 (over x, core).
Axes of the slice: x: 2, y: 2, z: 4, core: 2. Of those that a mesh axis runs over, the one named last changes fastest.
Arguments:
- query_rows: bfloat16 [2048, 2048], P('ep', 'tp'), may hold values from -6 to 6
- key_rows: bfloat16 [2048, 512], P('ep', 'tp'), may hold values from -18 to 18
- value_rows: bfloat16 [2048, 512], P('ep', 'tp'), may hold values from -12 to 12
- key_bias: bfloat16 [2048, 8], P('ep', 'tp'), may hold values from -2 to 13
- head_offset: float32 [32], P('tp'), may hold values from -16 to -3
- out_weight: bfloat16 [2048, 2048], P('tp'), may hold values from -0.125 to 0.125
- expert_input: bfloat16 [4096, 2048], P(('ep', 'tp')), may hold values from -40 to 40
- expert_gain: float32 [2048], replicated, may hold values from 0.1 to 1.9
- routes: int32 [4096, 2], P(('ep', 'tp')), may hold values from 0 to 7, all different within a row; in each aligned block of 128 rows (0 to 127, 128 to 255, ...) at most 48 rows name the same one
- route_weight: float32 [4096, 2], P(('ep', 'tp')), may hold values from 0.5 to 2
- gate_weight: bfloat16 [8, 2048, 3584], P('ep', None, 'tp'), may hold values from -0.125 to 0.125
- up_weight: bfloat16 [8, 2048, 3584], P('ep', None, 'tp'), may hold values from -0.125 to 0.125
- down_weight: bfloat16 [8, 3584, 2048], P('ep', 'tp'), may hold values from -0.09375 to 0.09375
Outputs:
- mixed_a: bfloat16 [2048, 2048], P(('ep', 'tp'))
- mixed_b: bfloat16 [4096, 2048], P(('ep', 'tp'))
The draws below stay inside these ranges and needn't reach their ends.
Inputs may be any that keep to these rules, and one draw needn't show every extreme that they name: `routes`: each row names 2 different experts; in the rows of one device (aligned blocks of 128 rows) no expert is named more than 48 times, and in every draw some device names some expert exactly 48 times.
All inputs are finite; a program needn't handle non-finite values.
Results may differ from the reference program's by a relative error of at most 0.012.
Values may be sent and summed in bfloat16 or wider, within the bound.
A program may use at most 128 MiB of HBM per device.

```python
import math
import jax
import jax.numpy as jnp
import numpy as np
from jax import lax

D = 2048
HEADS = 32
KEY_VALUE_HEADS = 8
HD = 64
FF = 3584
TOPK = 2
TOK_A = 256
TOK_B = 128
SEQUENCE_LEN_A = 2048
TOKENS_B = 4096
EXPERTS = 8
CAP = 48
N_EP = 8
N_TP = 4


def draw_head_offset(key, part):
    first_key, second_key, key_third_part = jax.random.split(jax.random.fold_in(key, 17), 3)
    picks = jax.random.randint(first_key, (HEADS,), 0, 8)
    slow_heads = picks < 4
    slow_value = -4.5 - math.log(SEQUENCE_LEN_A) + jax.random.uniform(second_key, (HEADS,), jnp.float32, -0.5, 0.5)
    fast_value = jax.random.uniform(key_third_part, (HEADS,), jnp.float32, -5.0, -3.0)
    return jnp.where(slow_heads, slow_value, fast_value).astype(jnp.float32)


def draw_key_bias(key, part):
    first_key, second_key, key_third_part = jax.random.split(jax.random.fold_in(key, 23), 3)
    spread = 0.8
    block_count = SEQUENCE_LEN_A // TOK_A
    factors = jax.random.uniform(first_key, (block_count, 1, KEY_VALUE_HEADS), jnp.float32, -spread, spread)
    factors = jnp.broadcast_to(factors, (block_count, TOK_A, KEY_VALUE_HEADS)).reshape(SEQUENCE_LEN_A, KEY_VALUE_HEADS)
    noise = 0.3 * jax.random.normal(second_key, (SEQUENCE_LEN_A, KEY_VALUE_HEADS), jnp.float32)
    start_offset = jnp.clip(factors + noise, -1.5, 1.5)
    group_position = jax.random.randint(key_third_part, (2, KEY_VALUE_HEADS), 0, SEQUENCE_LEN_A)
    token_group = jnp.any(jnp.arange(SEQUENCE_LEN_A)[:, None, None] == group_position[None, :, :], axis=1)
    return (start_offset + 11.0 * token_group.astype(jnp.float32)).astype(jnp.bfloat16)


def draw_expert_input(key, part):
    first_key, second_key = jax.random.split(jax.random.fold_in(key, 31), 2)
    scales = jnp.exp(jax.random.uniform(first_key, (TOKENS_B, 1), jnp.float32, 0.0, math.log(10.0)))
    values = jnp.clip(jax.random.normal(second_key, (TOKENS_B, D), jnp.float32), -4.0, 4.0)
    return (values * scales).astype(jnp.bfloat16)


def level_of(stream_key, dims, shards, low, high):
    level, own = 1.0, jax.random.fold_in(stream_key, 6)
    for position, blocks in shards:
        heights = jnp.exp(jax.random.uniform(jax.random.fold_in(own, position), (blocks,), jnp.float32, low / len(shards), high / len(shards)))
        level = level * jnp.repeat(heights, dims[position] // blocks).reshape([-1 if axis == position else 1 for axis in range(len(dims))])
    return level


def shared_out(own_key, own, number, rows, number_of, top, reach, slope):
    sequence = jax.random.permutation(own_key, number_of)
    heavy_load, usual = portions_of(number_of, rows * top, reach, slope, True), portions_of(number_of, rows * top, reach, slope, False)
    places = jnp.arange(number_of)

    def named(tallies, offset_by):
        used = int((tallies > 0).sum())
        fixed = max(1, used // 4)
        moved = fixed + (places - fixed + offset_by * (used - fixed)) % max(1, number_of - fixed)
        return jnp.zeros((number_of,), jnp.int32).at[sequence[jnp.where(places < fixed, places, moved)]].set(jnp.asarray(tallies, jnp.int32))

    tallies = jnp.where(number % 4 == 0, named(heavy_load, number // 4), named(usual, number - number // 4 - 1))
    mixed = jax.random.permutation(jax.random.fold_in(own, 3), number_of)
    source_of, taker = mixed[0:number_of // 2 * 2:2], mixed[1:number_of // 2 * 2:2]
    slack = jnp.minimum(tallies[source_of] - 1, reach - tallies[taker]) // 2
    slack = jnp.where((source_of == sequence[0]) | (taker == sequence[0]) | (tallies[taker] == 0), 0, jnp.maximum(slack, 0))
    moved = jax.random.randint(jax.random.fold_in(own, 4), (number_of // 2,), 0, 1 << 20) % (slack + 1)
    tallies = tallies.at[source_of].add(-moved).at[taker].add(moved)
    items = jnp.searchsorted(jnp.cumsum(tallies), jnp.arange(rows * top), side="right").astype(jnp.int32)
    listing = items.reshape(top, rows).T
    listing = listing[jax.random.permutation(jax.random.fold_in(own, 1), rows)]
    offset_by = jax.random.randint(jax.random.fold_in(own, 2), (rows, 1), 0, top)
    return jnp.take_along_axis(listing, (jnp.arange(top)[None, :] + offset_by) % top, axis=1)


def portions_of(number_of, total, most, slope, full):
    weights = [(1 << 20) // math.isqrt(standing ** slope) + 1 for standing in range(1, number_of + 1)]
    largest = most if full else min(most, max(-(-total // number_of), total * weights[0] // sum(weights)))
    least = 1 if total - largest >= number_of - 1 else 0
    given, surplus = [largest] + [least] * (number_of - 1), total - largest - least * (number_of - 1)
    while surplus > 0:
        free = [i for i in range(1, number_of) if given[i] < largest] or [i for i in range(1, number_of) if given[i] < most]
        pool, remaining = sum([weights[i] for i in free]), surplus
        for i in free:
            addition = min(most - given[i], max(1, remaining * weights[i] // pool), surplus)
            given[i] = given[i] + addition
            surplus = surplus - addition
    return np.array(given)


def normal_values(own_key, extent, scale, reach, cuts=(), kind=jnp.bfloat16):
    entries = jax.random.normal(own_key, extent, jnp.float32) * scale
    if len(cuts) > 0:
        entries = level_of(own_key, extent, cuts, -0.22, 0.18) * entries
    return jnp.clip(entries, min=-reach, max=reach).astype(kind)


def setup_inputs(seed: int = 0) -> dict:
    seeds = jax.random.split(jax.random.key(seed), 14)
    query_rows = normal_values(seeds[0], (SEQUENCE_LEN_A, HEADS * HD), 1.0, 6.0, ((0, 8), (1, 4)))
    key_rows = normal_values(seeds[1], (SEQUENCE_LEN_A, KEY_VALUE_HEADS * HD), 3.0, 18.0, ((0, 8), (1, 4)))
    value_rows = normal_values(seeds[2], (SEQUENCE_LEN_A, KEY_VALUE_HEADS * HD), 2.0, 12.0, ((0, 8), (1, 4)))
    key_bias = draw_key_bias(jax.random.fold_in(seeds[13], 71), 0)
    head_offset = draw_head_offset(jax.random.fold_in(seeds[13], 71), 0)
    out_weight = normal_values(seeds[5], (HEADS * HD, D), (HEADS * HD) ** -0.5, 0.125, ((0, 4),))
    expert_input = draw_expert_input(jax.random.fold_in(seeds[13], 71), 0)
    expert_gain = jnp.clip(1.0 + 0.18 * jax.random.normal(seeds[7], (D,), jnp.float32), 0.1, 1.9)
    routes_keys = jax.random.split(jax.random.fold_in(seeds[8], 1), TOKENS_B // TOK_B)
    routes_turns = jax.random.permutation(jax.random.fold_in(seeds[8], 3), TOKENS_B // TOK_B)
    routes = jax.vmap(lambda own, number: shared_out(jax.random.fold_in(seeds[8], 2), own, number, TOK_B, EXPERTS, TOPK, CAP, 1))(routes_keys, routes_turns).reshape((TOKENS_B, TOPK))
    route_weight = jnp.clip(0.5 + 1.5 * jax.random.uniform(seeds[9], (TOKENS_B, TOPK), jnp.float32) ** level_of(seeds[9], (TOKENS_B, TOPK), ((0, 32),), -0.2, 0.2), 0.5, 2.0)
    gate_weight = normal_values(seeds[10], (EXPERTS, D, FF), D ** -0.5, 0.125, ((0, 8), (2, 4)))
    up_weight = normal_values(seeds[11], (EXPERTS, D, FF), D ** -0.5, 0.125, ((0, 8), (2, 4)))
    down_weight = normal_values(seeds[12], (EXPERTS, FF, D), FF ** -0.5, 0.09375, ((0, 8), (1, 4)))
    return {"query_rows": query_rows, "key_rows": key_rows, "value_rows": value_rows, "key_bias": key_bias, "head_offset": head_offset, "out_weight": out_weight, "expert_input": expert_input, "expert_gain": expert_gain, "routes": routes, "route_weight": route_weight, "gate_weight": gate_weight, "up_weight": up_weight, "down_weight": down_weight}


EPSILON = 1e-06

def rms_normed(rows, gain):
    values = rows.astype(jnp.float32)
    scaled = values * lax.rsqrt(lax.optimization_barrier(jnp.mean(values * values, axis=-1, keepdims=True)) + EPSILON)
    return (scaled * gain).astype(jnp.bfloat16)

def stick_heads(query_rows, key_rows, value_rows, key_bias, head_offset):
    group_size = HEADS // KEY_VALUE_HEADS
    queries4 = query_rows.astype(jnp.float32).reshape(SEQUENCE_LEN_A, KEY_VALUE_HEADS, group_size, HD)
    key_heads = key_rows.astype(jnp.float32).reshape(SEQUENCE_LEN_A, KEY_VALUE_HEADS, HD)
    value_heads = value_rows.astype(jnp.float32).reshape(SEQUENCE_LEN_A, KEY_VALUE_HEADS, HD)
    offsets = head_offset.reshape(KEY_VALUE_HEADS, group_size)
    bias_rows = jnp.transpose(key_bias.astype(jnp.float32))
    block_rows = math.gcd(TOK_A, 128)
    key_pos = jnp.arange(SEQUENCE_LEN_A, dtype=jnp.int32)

    def one_block(block_turn):
        first_row = (block_turn * block_rows).astype(jnp.int32)
        query_block = lax.dynamic_slice_in_dim(queries4, first_row, block_rows, 0)
        scores = jnp.einsum('qgjd,kgd->gjqk', query_block, key_heads) * (1.0 / math.sqrt(HD))
        scores = scores + offsets[:, :, None, None] + bias_rows[:, None, None, :]
        query_pos = first_row + jnp.arange(block_rows, dtype=jnp.int32)
        keep_mask = key_pos[None, :] < query_pos[:, None]
        log_stay = jnp.where(keep_mask, jax.nn.log_sigmoid(-scores), 0.0)
        after_sum = lax.cumsum(log_stay, axis=3, reverse=True) - log_stay
        weights = jnp.where(keep_mask, jnp.exp(jax.nn.log_sigmoid(scores) + after_sum), 0.0).astype(jnp.bfloat16)
        weights = lax.optimization_barrier(weights).astype(jnp.float32)
        return jnp.einsum('gjqk,kgd->qgjd', weights, value_heads).reshape(block_rows, HEADS * HD)
    blocks = lax.map(one_block, jnp.arange(SEQUENCE_LEN_A // block_rows, dtype=jnp.int32))
    return blocks.reshape(SEQUENCE_LEN_A, HEADS * HD).astype(jnp.bfloat16)

def reference(query_rows, key_rows, value_rows, key_bias, head_offset, out_weight, expert_input, expert_gain, routes, route_weight, gate_weight, up_weight, down_weight):
    heads_out = stick_heads(query_rows, key_rows, value_rows, key_bias, head_offset)
    col_part = HEADS * HD // N_TP
    total_sum = jnp.zeros((SEQUENCE_LEN_A, D), jnp.float32)
    for tp_part in range(N_TP):
        lower = tp_part * col_part
        partial_value = jnp.dot(heads_out[:, lower:lower + col_part], out_weight[lower:lower + col_part], preferred_element_type=jnp.float32).astype(jnp.bfloat16)
        total_sum = total_sum + lax.optimization_barrier(partial_value).astype(jnp.float32)
    mixed_a = total_sum.astype(jnp.bfloat16)
    normed = rms_normed(expert_input, expert_gain)
    flat_route = routes.reshape(-1)
    flat_token = (jnp.arange(TOKENS_B * TOPK, dtype=jnp.int32) // TOPK).astype(jnp.int32)
    flattened_weight = route_weight.reshape(-1)
    row_limit = N_EP * N_TP * CAP
    hidden_part = FF // N_TP

    def one_expert(expert_id):
        order_rows = jnp.argsort((flat_route != expert_id).astype(jnp.int32), stable=True)[:row_limit].astype(jnp.int32)
        live = flat_route[order_rows] == expert_id
        inputs = normed[flat_token[order_rows]]
        gate_act = jnp.dot(inputs, gate_weight[expert_id], preferred_element_type=jnp.float32)
        up_act = jnp.dot(inputs, up_weight[expert_id], preferred_element_type=jnp.float32)
        hidden = (jax.nn.silu(gate_act) * up_act).astype(jnp.bfloat16)
        down_rows = down_weight[expert_id]
        expert_sum = jnp.zeros((row_limit, D), jnp.float32)
        for tp_part in range(N_TP):
            lower = tp_part * hidden_part
            partial_value = jnp.dot(hidden[:, lower:lower + hidden_part], down_rows[lower:lower + hidden_part], preferred_element_type=jnp.float32).astype(jnp.bfloat16)
            expert_sum = expert_sum + lax.optimization_barrier(partial_value).astype(jnp.float32)
        result = lax.optimization_barrier(expert_sum.astype(jnp.bfloat16)).astype(jnp.float32)
        scaled = result * jnp.where(live, flattened_weight[order_rows], 0.0)[:, None]
        return (order_rows, scaled)
    orders, results = lax.map(one_expert, jnp.arange(EXPERTS, dtype=jnp.int32))
    combined = jnp.zeros((TOKENS_B, D), jnp.float32).at[flat_token[orders.reshape(-1)]].add(results.reshape(-1, D))
    mixed_b = combined.astype(jnp.bfloat16)
    return (mixed_a, mixed_b)
```

```python
import functools
import math

import jax
import jax.numpy as jnp
from jax import lax
from jax.experimental import pallas as pl
from jax.experimental.pallas import tpu as pltpu
from jax.sharding import PartitionSpec as P

HD = 64
EPSILON = 1e-06
LOG2E = 1.4426950408889634
MESH = pl.DeviceIdType.MESH
CORES = 2
AHEAD = 3


def xor(a, b, size):
    total, bit = 0, 1
    while bit < size:
        total = total + bit * ((a // bit + b // bit) % 2)
        bit *= 2
    return total


def step_kernel(
    q_ref, k_ref, v_ref, bias_ref, offset_ref, x_ref, gain_ref, slot_rows_ref, slot_cols_ref, mix_ref,
    wo_hbm, wg_hbm, wu_hbm, wd_hbm,
    out_a_ref, out_b_ref,
    qw, kbuf, vbuf, bbuf, acc, carry, heads_out, tri,
    outgoing, rows, hidden, part, got, sum_out, sum_in, back_out, back_in,
    part_a, got_a, sum_out_a, sum_in_a,
    wgu, wd, wo,
    w_sem, kv_zsend, kv_psend, kv_recv,
    d_send, d_recv, x_send, x_recv, c_send, c_recv, p_send, p_recv, s_send, s_recv, b_send, b_recv,
    a_send, a_recv,
    *, ep, chunks, group_size, kv_local,
):
    me = lax.axis_index("ep")
    t = lax.axis_index("tp")
    c = t % CORES
    x = t // CORES
    mate = {"tp": CORES * x + 1 - c}
    across = {"tp": CORES * (1 - x) + c}
    per = ep // chunks
    cap = outgoing.shape[1]
    width = outgoing.shape[2]
    block = k_ref.shape[0]
    heads = kv_local * group_size
    up = me // 2
    upper = ep // 2
    odd = me % 2
    pair = me + 1 - 2 * odd

    def remote(src, dst, send, recv, device):
        return pltpu.make_async_remote_copy(
            src_ref=src, dst_ref=dst, send_sem=send, recv_sem=recv, device_id=device, device_id_type=MESH
        )

    tiles = wgu.shape[0]
    half = wgu.shape[2] // 2

    def weight_copies():
        copies = []
        for tile in range(tiles):
            lanes = slice(tile * half, (tile + 1) * half)
            copies.append(pltpu.make_async_copy(wg_hbm.at[0, :, lanes], wgu.at[tile, :, 0:half], w_sem.at[2 * tile]))
            copies.append(
                pltpu.make_async_copy(wu_hbm.at[0, :, lanes], wgu.at[tile, :, half : 2 * half], w_sem.at[2 * tile + 1])
            )
        copies.append(pltpu.make_async_copy(wd_hbm.at[0], wd, w_sem.at[2 * tiles]))
        return copies

    wo_copy = pltpu.make_async_copy(wo_hbm, wo, w_sem.at[2 * tiles + 1])
    wo_copy.start()
    for copy in weight_copies():
        copy.start()

    barrier = pltpu.get_barrier_semaphore()

    def greet(step, unused):
        pl.semaphore_signal(barrier, inc=1, device_id={"ep": (me + step) % ep}, device_id_type=MESH)
        return unused

    lax.fori_loop(1, ep, greet, 0)
    pl.semaphore_signal(barrier, inc=1, device_id=mate, device_id_type=MESH)
    pl.semaphore_signal(barrier, inc=1, device_id=across, device_id_type=MESH)
    pl.semaphore_wait(barrier, ep + 1)

    def own_kv(target, sems):
        return [
            remote(k_ref, kbuf.at[me], sems.at[0], kv_recv.at[me, 0], {"ep": target}),
            remote(v_ref, vbuf.at[me], sems.at[1], kv_recv.at[me, 1], {"ep": target}),
            remote(bias_ref, bbuf.at[me], sems.at[2], kv_recv.at[me, 2], {"ep": target}),
        ]

    def passed_kv(source, target):
        return [
            remote(ref.at[source], ref.at[source], kv_psend.at[source, i], kv_recv.at[source, i], {"ep": target})
            for i, ref in enumerate((kbuf, vbuf, bbuf))
        ]

    @pl.when(odd == 0)
    def _():
        for copy in own_kv(pair, kv_psend.at[me]):
            copy.start()

    def send_up(step, unused):
        for copy in own_kv(me + 2 * step, kv_zsend.at[step]):
            copy.start()
        return unused

    lax.fori_loop(1, upper - up, send_up, 0)

    values = x_ref[...].astype(jnp.float32)
    scale = lax.rsqrt(jnp.mean(values * values, axis=-1, keepdims=True) + EPSILON)
    normed = (values * scale * gain_ref[...]).astype(jnp.bfloat16)
    tok = normed.shape[0]
    ids = lax.broadcasted_iota(jnp.int32, (ep * cap, tok), 0)
    hit = (ids == slot_rows_ref[0:1, :]) | (ids == slot_rows_ref[1:2, :])
    hit = jnp.where(hit, 1.0, 0.0).astype(jnp.bfloat16)
    strip = 512
    for lane in range(0, width, strip):
        picked = jnp.dot(hit, normed[:, lane : lane + strip], preferred_element_type=jnp.float32)
        outgoing[:, :, lane : lane + strip] = picked.astype(jnp.bfloat16).reshape(ep, cap, strip)
    rows[0, c, 0, x] = outgoing[0]

    def slot_of(d):
        return rows.at[d // per, c, d % per, x]

    def dispatch(d):
        return remote(outgoing.at[d], slot_of(d), d_send.at[d], d_recv.at[d], {"ep": xor(me, d, ep)})

    def issue(d, unused):
        dispatch(d).start()
        return unused

    lax.fori_loop(1, 1 + AHEAD, issue, 0)

    lane_ids = lax.broadcasted_iota(jnp.int32, (kv_local * HD, kv_local * HD), 1)
    row_ids = lax.broadcasted_iota(jnp.int32, (kv_local * HD, kv_local * HD), 0)
    wide = kv_local * HD
    for head in range(heads):
        kv = head // group_size
        first = head * HD // wide * wide
        shift = head * HD - first - kv * HD
        move = jnp.where((row_ids == lane_ids + shift) & (lane_ids // HD == kv), 1.0, 0.0).astype(jnp.bfloat16)
        qw[head] = jnp.dot(
            q_ref[:, first : first + wide], move, preferred_element_type=jnp.float32
        ).astype(jnp.bfloat16)
    key_ids = lax.broadcasted_iota(jnp.int32, (block, block), 0)
    place = lax.broadcasted_iota(jnp.int32, (block, block), 1)
    tri[...] = jnp.where(key_ids > place, 1.0, 0.0).astype(jnp.bfloat16)
    acc[...] = jnp.zeros_like(acc)
    carry[...] = jnp.zeros_like(carry)

    def tile(keys, vals, biases, keep):
        for head in range(heads):
            kv = head // group_size
            raw = lax.dot_general(
                qw[head], keys[...], (((1,), (1,)), ((), ())), preferred_element_type=jnp.float32
            )
            row = (biases[kv : kv + 1, :].astype(jnp.float32) + offset_ref[head]) * LOG2E
            scores = raw * (LOG2E / math.sqrt(HD)) + row
            soft = jnp.log2(1.0 + jnp.exp2(-jnp.abs(scores)))
            leave = jnp.maximum(scores, 0.0) + soft
            log_take = jnp.minimum(scores, 0.0) - soft
            if keep is not None:
                leave = jnp.where(keep, leave, 0.0)
            high = leave.astype(jnp.bfloat16)
            low = (leave - high.astype(jnp.float32)).astype(jnp.bfloat16)
            after = jnp.dot(high, tri[...], preferred_element_type=jnp.float32) + jnp.dot(
                low, tri[...], preferred_element_type=jnp.float32
            )
            before = carry[head]
            weights = jnp.exp2(log_take - after - before)
            if keep is not None:
                weights = jnp.where(keep, weights, 0.0)
            acc[head] += jnp.dot(weights.astype(jnp.bfloat16), vals[...], preferred_element_type=jnp.float32)
            carry[head] = before + after[:, :1] + leave[:, :1]

    def wait_kv(source):
        for i, ref in enumerate((kbuf, vbuf, bbuf)):
            remote(ref.at[source], ref.at[source], kv_psend.at[source, i], kv_recv.at[source, i], mate).wait_recv()

    def project():
        lanes = slice(0, 0)
        pieces = []
        for head in range(heads):
            kv = head // group_size
            lanes = slice(kv * HD, (kv + 1) * HD)
            pieces.append(acc[head, :, lanes].astype(jnp.bfloat16))
        for head in range(heads):
            heads_out[:, head * HD : (head + 1) * HD] = pieces[head]
        own = part_a.shape[2]
        for lane in range(0, width, strip):
            value = jnp.dot(heads_out[...], wo[:, lane : lane + strip], preferred_element_type=jnp.float32)
            value = value.astype(jnp.bfloat16).reshape(2, CORES, own, strip)
            for xs in range(2):
                for cs in range(CORES):
                    part_a[cs, xs, :, lane : lane + strip] = value[xs, cs]

    def send_a():
        return remote(part_a.at[1 - c], got_a, a_send.at[0], a_recv.at[0], mate)

    def cross_a():
        return remote(sum_out_a, sum_in_a, a_send.at[1], a_recv.at[1], across)

    def experts(k):
        flat_rows = part.shape[1] * part.shape[2] * part.shape[3] * cap

        def gate_up(j, unused):
            both = jnp.dot(
                rows[k].reshape(flat_rows, width), wgu[j], preferred_element_type=jnp.float32
            )
            gate = both[:, :half]
            hidden[:, pl.ds(pl.multiple_of(j * half, half), half)] = (
                gate / (1.0 + jnp.exp(-gate)) * both[:, half:]
            ).astype(jnp.bfloat16)
            return unused

        lax.fori_loop(0, tiles, gate_up, 0)

        def down(j, unused):
            lanes = pl.ds(pl.multiple_of(j * strip, strip), strip)
            value = jnp.dot(hidden[...], wd[:, lanes], preferred_element_type=jnp.float32)
            part[k, :, :, :, :, lanes] = value.astype(jnp.bfloat16).reshape(part.shape[1:5] + (strip,))
            return unused

        lax.fori_loop(0, width // strip, down, 0)

    def send_p(k):
        return remote(part.at[k, 1 - c], got.at[k], p_send.at[k], p_recv.at[k], mate)

    def cross_p(k):
        return remote(sum_out.at[k], sum_in.at[k], s_send.at[k], s_recv.at[k], across)

    def send_back(k, i):
        d = k * per + i
        return remote(back_out.at[d], back_in.at[d], b_send.at[d], b_recv.at[d], {"ep": xor(me, d, ep)})

    def forward_x(d):
        return remote(slot_of(d), slot_of(d), x_send.at[d], x_recv.at[d], across)

    def forward_c(d):
        return remote(slot_of(d), slot_of(d), c_send.at[d, 0], c_recv.at[d, 0], mate)

    def forward_xc(d):
        ref = rows.at[d // per, c, d % per, 1 - x]
        return remote(ref, ref, c_send.at[d, 1], c_recv.at[d, 1], mate)

    first_chunk = per + 1

    def step(i, unused):
        @pl.when(i < ep)
        def _():
            @pl.when(i > 0)
            def _():
                dispatch(i).wait_recv()

            forward_x(i).start()
            forward_c(i).start()

        @pl.when((i > 0) & (i <= ep))
        def _():
            forward_x(i - 1).wait_recv()
            forward_xc(i - 1).start()

        @pl.when(i + AHEAD + 1 < ep)
        def _():
            dispatch(i + AHEAD + 1).start()

        lag = i - first_chunk - 2
        @pl.when((lag >= 0) & (lag % per == 0) & (lag // per < chunks))
        def _():
            k = lag // per
            cross_p(k).wait_recv()

            def finish(n, unused):
                total = (
                    part[k, c, n, x].astype(jnp.float32)
                    + got[k, n, x].astype(jnp.float32)
                    + sum_in[k, n].astype(jnp.float32)
                )
                back_out[k * per + n] = total.astype(jnp.bfloat16)

                @pl.when(k * per + n > 0)
                def _():
                    send_back(k, n).start()

                return unused

            lax.fori_loop(0, per, finish, 0)

        lag1 = i - first_chunk - 1
        @pl.when((lag1 >= 0) & (lag1 % per == 0) & (lag1 // per < chunks))
        def _():
            k = lag1 // per
            send_p(k).wait_recv()

            def add(n, unused):
                total = part[k, c, n, 1 - x].astype(jnp.float32) + got[k, n, 1 - x].astype(jnp.float32)
                sum_out[k, n] = total.astype(jnp.bfloat16)
                return unused

            lax.fori_loop(0, per, add, 0)
            cross_p(k).start()

        @pl.when(i == 0)
        def _():
            tile(k_ref, v_ref, bias_ref, place < key_ids)

        @pl.when((i > 0) & (i <= me))
        def _():
            source = me - i

            @pl.when(i % 2 == 1)
            def _():
                wait_kv(source)

            tile(kbuf.at[source], vbuf.at[source], bbuf.at[source], None)

        @pl.when((i % 2 == 0) & (i + 2 <= me))
        def _():
            wait_kv(me - i - 2)
            for copy in passed_kv(me - i - 2, pair):
                copy.start()

        @pl.when(i == me)
        def _():
            wo_copy.wait()
            project()
            send_a().start()

        @pl.when(i == me + 1)
        def _():
            send_a().wait_recv()
            sum_out_a[...] = (
                part_a[c, 1 - x].astype(jnp.float32) + got_a[1 - x].astype(jnp.float32)
            ).astype(jnp.bfloat16)
            cross_a().start()

        @pl.when(i == me + 3)
        def _():
            cross_a().wait_recv()
            out_a_ref[...] = (
                part_a[c, x].astype(jnp.float32) + got_a[x].astype(jnp.float32) + sum_in_a[...].astype(jnp.float32)
            ).astype(jnp.bfloat16)

        lag0 = i - first_chunk
        @pl.when((lag0 >= 0) & (lag0 % per == 0) & (lag0 // per < chunks))
        def _():
            k = lag0 // per

            @pl.when(k == 0)
            def _():
                for copy in weight_copies():
                    copy.wait()

            def landed(n, unused):
                forward_c(k * per + n).wait_recv()
                forward_xc(k * per + n).wait_recv()
                return unused

            lax.fori_loop(0, per, landed, 0)
            experts(k)
            send_p(k).start()

        return unused

    lax.fori_loop(0, first_chunk + (chunks - 1) * per + 3, step, 0)

    back_in[0] = back_out[0]

    def returned(d, unused):
        remote(back_out.at[d], back_in.at[d], b_send.at[d], b_recv.at[d], mate).wait_recv()
        return unused

    lax.fori_loop(1, ep, returned, 0)
    spots = lax.broadcasted_iota(jnp.int32, (tok, ep * cap), 1)
    share = jnp.zeros((tok, ep * cap), jnp.float32)
    for choice in range(slot_cols_ref.shape[1]):
        share = share + jnp.where(spots == slot_cols_ref[:, choice : choice + 1], mix_ref[:, choice : choice + 1], 0.0)
    high = share.astype(jnp.bfloat16)
    rest = share - high.astype(jnp.float32)
    low = rest.astype(jnp.bfloat16)
    for lane in range(0, width, strip):
        piece = back_in[:, :, lane : lane + strip].reshape(ep * cap, strip)
        out_b_ref[:, lane : lane + strip] = (
            jnp.dot(high, piece, preferred_element_type=jnp.float32)
            + jnp.dot(low, piece, preferred_element_type=jnp.float32)
        ).astype(jnp.bfloat16)

    @pl.when(odd == 0)
    def _():
        for copy in own_kv(pair, kv_psend.at[me]):
            copy.wait_send()

    def left_up(step, unused):
        for copy in own_kv(me + 2 * step, kv_zsend.at[step]):
            copy.wait_send()
        return unused

    lax.fori_loop(1, upper - up, left_up, 0)

    def left_pair(step, unused):
        for copy in passed_kv(me - 2 * step, pair):
            copy.wait_send()
        return unused

    lax.fori_loop(1, up + 1, left_pair, 0)

    def left_rows(d, unused):
        @pl.when(d > 0)
        def _():
            dispatch(d).wait_send()
            send_back(d // per, d % per).wait_send()

        forward_x(d).wait_send()
        forward_c(d).wait_send()
        forward_xc(d).wait_send()
        return unused

    lax.fori_loop(0, ep, left_rows, 0)

    def left_sums(k, unused):
        send_p(k).wait_send()
        cross_p(k).wait_send()
        return unused

    lax.fori_loop(0, chunks, left_sums, 0)
    send_a().wait_send()
    cross_a().wait_send()


def body(
    query_rows,
    key_rows,
    value_rows,
    key_bias,
    head_offset,
    out_weight,
    expert_input,
    expert_gain,
    routes,
    route_weight,
    gate_weight,
    up_weight,
    down_weight,
):
    ep, tp = lax.axis_size("ep"), lax.axis_size("tp")
    me = lax.axis_index("ep")
    block = key_rows.shape[0]
    kv_local = key_rows.shape[1] // HD
    heads = query_rows.shape[1] // HD
    tok, width = expert_input.shape
    top = routes.shape[1]
    hidden_width = gate_weight.shape[2]
    cap = max(2, 3 * tok * top // (2 * ep))
    cap = -(-cap // 16) * 16
    chunks = 4
    per = ep // chunks
    across = tp // CORES
    flat = routes.reshape(-1)
    order = jnp.arange(flat.shape[0])
    rank = jnp.sum((flat[:, None] == flat[None, :]) & (order[None, :] < order[:, None]), axis=1, dtype=jnp.int32)
    slots = ((flat ^ me) * cap + rank).reshape(tok, top)
    bias = jnp.pad(key_bias.T, ((0, 16 - kv_local), (0, 0)))
    half = 128
    tiles = hidden_width // half
    vmem = pl.BlockSpec(memory_space=pltpu.VMEM)
    hbm = pl.BlockSpec(memory_space=pl.ANY)
    bf16, f32, dma = jnp.bfloat16, jnp.float32, pltpu.SemaphoreType.DMA
    own_a = block // tp
    wide = kv_local * HD
    return pl.pallas_call(
        functools.partial(step_kernel, ep=ep, chunks=chunks, group_size=heads // kv_local, kv_local=kv_local),
        out_shape=(
            jax.ShapeDtypeStruct((own_a, width), bf16),
            jax.ShapeDtypeStruct((tok, width), bf16),
        ),
        in_specs=[vmem] * 4 + [pl.BlockSpec(memory_space=pltpu.SMEM)] + [vmem] * 5 + [hbm] * 4,
        out_specs=(vmem, vmem),
        scratch_shapes=[
            pltpu.VMEM((heads, block, wide), bf16),
            pltpu.VMEM((ep, block, wide), bf16),
            pltpu.VMEM((ep, block, wide), bf16),
            pltpu.VMEM((ep, 16, block), bf16),
            pltpu.VMEM((heads, block, wide), f32),
            pltpu.VMEM((heads, block, 1), f32),
            pltpu.VMEM((block, heads * HD), bf16),
            pltpu.VMEM((block, block), bf16),
            pltpu.VMEM((ep, cap, width), bf16),
            pltpu.VMEM((chunks, CORES, per, across, cap, width), bf16),
            pltpu.VMEM((CORES * per * across * cap, hidden_width), bf16),
            pltpu.VMEM((chunks, CORES, per, across, cap, width), bf16),
            pltpu.VMEM((chunks, per, across, cap, width), bf16),
            pltpu.VMEM((chunks, per, cap, width), bf16),
            pltpu.VMEM((chunks, per, cap, width), bf16),
            pltpu.VMEM((ep, cap, width), bf16),
            pltpu.VMEM((ep, cap, width), bf16),
            pltpu.VMEM((CORES, across, own_a, width), bf16),
            pltpu.VMEM((across, own_a, width), bf16),
            pltpu.VMEM((own_a, width), bf16),
            pltpu.VMEM((own_a, width), bf16),
            pltpu.VMEM((tiles, width, 2 * half), bf16),
            pltpu.VMEM((hidden_width, width), bf16),
            pltpu.VMEM((heads * HD, width), bf16),
            dma((2 * tiles + 2,)),
            dma((ep // 2, 3)),
            dma((ep, 3)),
            dma((ep, 3)),
            dma((ep,)), dma((ep,)), dma((ep,)), dma((ep,)), dma((ep, 2)), dma((ep, 2)),
            dma((chunks,)), dma((chunks,)), dma((chunks,)), dma((chunks,)), dma((ep,)), dma((ep,)),
            dma((2,)), dma((2,)),
        ],
        compiler_params=pltpu.CompilerParams(
            collective_id=0, has_side_effects=True, vmem_limit_bytes=60 * 1024 * 1024
        ),
        name="step",
    )(
        query_rows, key_rows, value_rows, bias, head_offset, expert_input, expert_gain[None, :],
        slots.T, slots, route_weight, out_weight, gate_weight, up_weight, down_weight,
    )


def solution(mesh):
    return jax.shard_map(
        body,
        mesh=mesh,
        in_specs=(
            P("ep", "tp"),
            P("ep", "tp"),
            P("ep", "tp"),
            P("ep", "tp"),
            P("tp"),
            P("tp", None),
            P(("ep", "tp"), None),
            P(),
            P(("ep", "tp"), None),
            P(("ep", "tp"), None),
            P("ep", None, "tp"),
            P("ep", None, "tp"),
            P("ep", "tp", None),
        ),
        out_specs=(P(("ep", "tp"), None), P(("ep", "tp"), None)),
        check_vma=False,
    )
```

```python
import functools
import math

import jax
import jax.numpy as jnp
from jax import lax
from jax.experimental import pallas as pl
from jax.experimental.pallas import tpu as pltpu
from jax.sharding import PartitionSpec as P

HD = 64
EPSILON = 1e-06
LOG2E = 1.4426950408889634
MESH = pl.DeviceIdType.MESH
CORES = 2


def xor(a, b, size):
    total, bit = 0, 1
    while bit < size:
        total = total + bit * ((a // bit + b // bit) % 2)
        bit *= 2
    return total


def step_kernel(
    q_ref, k_ref, v_ref, bias_ref, offset_ref, x_ref, gain_ref, routes_ref, mix_ref,
    wo_hbm, wg_hbm, wu_hbm, wd_hbm,
    out_a_ref, out_b_ref,
    qw, kbuf, vbuf, bbuf, acc, carry, heads_out, tri,
    hit, share_high, share_low, outgoing, rows, hidden, part, got, sum_out, sum_in, back_out, back_in,
    part_a, got_a, sum_out_a, sum_in_a,
    wgu, wd, wo,
    w_sem, kv_zsend, kv_psend, kv_recv,
    d_send, d_recv, x_send, x_recv, c_send, c_recv, p_send, p_recv, s_send, s_recv, b_send, b_recv,
    a_send, a_recv,
    *, ep, chunks, group_size, kv_local,
):
    me = lax.axis_index("ep")
    t = lax.axis_index("tp")
    c = t % CORES
    x = t // CORES
    mate = {"tp": CORES * x + 1 - c}
    across = {"tp": CORES * (1 - x) + c}
    per = ep // chunks
    unit = per // 2
    cap = outgoing.shape[1]
    width = outgoing.shape[2]
    block = k_ref.shape[0]
    heads = kv_local * group_size
    up = me // 2
    upper = ep // 2
    odd = me % 2
    pair = me + 1 - 2 * odd

    def remote(src, dst, send, recv, device):
        return pltpu.make_async_remote_copy(
            src_ref=src, dst_ref=dst, send_sem=send, recv_sem=recv, device_id=device, device_id_type=MESH
        )

    tiles = wgu.shape[0]
    half = wgu.shape[2] // 2

    def weight_copies():
        copies = []
        for tile in range(tiles):
            lanes = slice(tile * half, (tile + 1) * half)
            copies.append(pltpu.make_async_copy(wg_hbm.at[0, :, lanes], wgu.at[tile, :, 0:half], w_sem.at[2 * tile]))
            copies.append(
                pltpu.make_async_copy(wu_hbm.at[0, :, lanes], wgu.at[tile, :, half : 2 * half], w_sem.at[2 * tile + 1])
            )
        copies.append(pltpu.make_async_copy(wd_hbm.at[0], wd, w_sem.at[2 * tiles]))
        return copies

    wo_copy = pltpu.make_async_copy(wo_hbm, wo, w_sem.at[2 * tiles + 1])
    wo_copy.start()
    for copy in weight_copies():
        copy.start()

    direct = range(1, per + per // 2)
    barrier = pltpu.get_barrier_semaphore()

    def greet(step, unused):
        pl.semaphore_signal(barrier, inc=1, device_id={"ep": (me + step) % ep}, device_id_type=MESH)
        return unused

    lax.fori_loop(1, ep, greet, 0)
    pl.semaphore_signal(barrier, inc=1, device_id=mate, device_id_type=MESH)
    pl.semaphore_signal(barrier, inc=1, device_id=across, device_id_type=MESH)
    for d in direct:
        device = {"ep": xor(me, d, ep), "tp": CORES * (1 - x) + c}
        pl.semaphore_signal(barrier, inc=1, device_id=device, device_id_type=MESH)

    values = x_ref[...].astype(jnp.float32)
    scale = lax.rsqrt(jnp.mean(values * values, axis=-1, keepdims=True) + EPSILON)
    normed = (values * scale * gain_ref[...]).astype(jnp.bfloat16)
    tok = normed.shape[0]
    bf16 = jnp.bfloat16
    expert_ids = xor(lax.broadcasted_iota(jnp.int32, (ep, tok), 0), me, ep)
    named = jnp.where((routes_ref[0:1, :] == expert_ids) | (routes_ref[1:2, :] == expert_ids), 1.0, 0.0)
    earlier = lax.broadcasted_iota(jnp.int32, (tok, tok), 0) < lax.broadcasted_iota(jnp.int32, (tok, tok), 1)
    rank = jnp.dot(named.astype(bf16), jnp.where(earlier, 1.0, 0.0).astype(bf16), preferred_element_type=jnp.float32)
    rank = jnp.where(named > 0.0, rank, -1.0)
    spots = lax.broadcasted_iota(jnp.int32, (cap, tok), 0).astype(jnp.float32)
    for d in range(ep):
        hit[d] = jnp.where(rank[d : d + 1, :] == spots, 1.0, 0.0).astype(bf16)
    strip = 512
    for lane in range(0, width, strip):
        picked = jnp.dot(hit[...].reshape(ep * cap, tok), normed[:, lane : lane + strip], preferred_element_type=jnp.float32)
        outgoing[:, :, lane : lane + strip] = picked.astype(jnp.bfloat16).reshape(ep, cap, strip)
    rows[0, c, 0, x] = outgoing[0]

    lane_ids = lax.broadcasted_iota(jnp.int32, (kv_local * HD, kv_local * HD), 1)
    row_ids = lax.broadcasted_iota(jnp.int32, (kv_local * HD, kv_local * HD), 0)
    wide = kv_local * HD
    for head in range(heads):
        kv = head // group_size
        first = head * HD // wide * wide
        shift = head * HD - first - kv * HD
        move = jnp.where((row_ids == lane_ids + shift) & (lane_ids // HD == kv), 1.0, 0.0).astype(jnp.bfloat16)
        qw[head] = jnp.dot(
            q_ref[:, first : first + wide], move, preferred_element_type=jnp.float32
        ).astype(jnp.bfloat16)
    key_ids = lax.broadcasted_iota(jnp.int32, (block, block), 0)
    place = lax.broadcasted_iota(jnp.int32, (block, block), 1)
    tri[...] = jnp.where(key_ids > place, 1.0, 0.0).astype(jnp.bfloat16)
    acc[...] = jnp.zeros_like(acc)
    carry[...] = jnp.zeros_like(carry)

    pl.semaphore_wait(barrier, ep + 1 + len(direct))

    def own_kv(target, sems):
        return [
            remote(k_ref, kbuf.at[me], sems.at[0], kv_recv.at[me, 0], {"ep": target}),
            remote(v_ref, vbuf.at[me], sems.at[1], kv_recv.at[me, 1], {"ep": target}),
            remote(bias_ref, bbuf.at[me], sems.at[2], kv_recv.at[me, 2], {"ep": target}),
        ]

    def passed_kv(source, target, sems):
        return [
            remote(ref.at[source], ref.at[source], sems.at[source, i], kv_recv.at[source, i], {"ep": target})
            for i, ref in enumerate((kbuf, vbuf, bbuf))
        ]

    @pl.when(odd == 0)
    def _():
        for copy in own_kv(pair, kv_psend.at[me]):
            copy.start()

    @pl.when(up < upper - 1)
    def _():
        for copy in own_kv(me + 2, kv_zsend.at[me]):
            copy.start()

    groups = [range(k * per, (k + 1) * per) for k in range(chunks)]

    def slot_of(d):
        return rows.at[d // per, c, d % per, x]

    def dispatch(d):
        return remote(outgoing.at[d], slot_of(d), d_send.at[d], d_recv.at[d], {"ep": xor(me, d, ep)})

    def dispatch_across(d):
        device = {"ep": xor(me, d, ep), "tp": CORES * (1 - x) + c}
        return remote(outgoing.at[d], slot_of(d), x_send.at[d], x_recv.at[d], device)

    def forward_x(d):
        return remote(slot_of(d), slot_of(d), x_send.at[d], x_recv.at[d], across)

    def forward_c(d):
        return remote(slot_of(d), slot_of(d), c_send.at[d, 0], c_recv.at[d, 0], mate)

    def forward_xc(d):
        ref = rows.at[d // per, c, d % per, 1 - x]
        return remote(ref, ref, c_send.at[d, 1], c_recv.at[d, 1], mate)

    forward_x(0).start()
    forward_c(0).start()
    for d in list(groups[0][1:]) + [d for pair_of in zip(groups[2], groups[1]) for d in pair_of]:
        dispatch(d).start()
        if d in direct:
            dispatch_across(d).start()

    def tile(keys, vals, biases, keep):
        for head in range(heads):
            kv = head // group_size
            raw = lax.dot_general(
                qw[head], keys[...], (((1,), (1,)), ((), ())), preferred_element_type=jnp.float32
            )
            row = (biases[kv : kv + 1, :].astype(jnp.float32) + offset_ref[head]) * LOG2E
            scores = raw * (LOG2E / math.sqrt(HD)) + row
            soft = jnp.log2(1.0 + jnp.exp2(-jnp.abs(scores)))
            leave = jnp.maximum(scores, 0.0) + soft
            log_take = jnp.minimum(scores, 0.0) - soft
            if keep is not None:
                leave = jnp.where(keep, leave, 0.0)
            high = leave.astype(jnp.bfloat16)
            low = (leave - high.astype(jnp.float32)).astype(jnp.bfloat16)
            after = jnp.dot(high, tri[...], preferred_element_type=jnp.float32) + jnp.dot(
                low, tri[...], preferred_element_type=jnp.float32
            )
            before = carry[head]
            weights = jnp.exp2(log_take - after - before)
            if keep is not None:
                weights = jnp.where(keep, weights, 0.0)
            acc[head] += jnp.dot(weights.astype(jnp.bfloat16), vals[...], preferred_element_type=jnp.float32)
            carry[head] = before + after[:, :1] + leave[:, :1]

    def wait_kv(source):
        for i, ref in enumerate((kbuf, vbuf, bbuf)):
            remote(ref.at[source], ref.at[source], kv_psend.at[source, i], kv_recv.at[source, i], mate).wait_recv()

    def project():
        lanes = slice(0, 0)
        pieces = []
        for head in range(heads):
            kv = head // group_size
            lanes = slice(kv * HD, (kv + 1) * HD)
            pieces.append(acc[head, :, lanes].astype(jnp.bfloat16))
        for head in range(heads):
            heads_out[:, head * HD : (head + 1) * HD] = pieces[head]
        own = part_a.shape[2]
        for lane in range(0, width, strip):
            value = jnp.dot(heads_out[...], wo[:, lane : lane + strip], preferred_element_type=jnp.float32)
            value = value.astype(jnp.bfloat16).reshape(2, CORES, own, strip)
            for xs in range(2):
                for cs in range(CORES):
                    part_a[cs, xs, :, lane : lane + strip] = value[xs, cs]

    def send_a():
        return remote(part_a.at[1 - c], got_a, a_send.at[0], a_recv.at[0], mate)

    def cross_a():
        return remote(sum_out_a, sum_in_a, a_send.at[1], a_recv.at[1], across)

    def experts(k):
        flat_rows = part.shape[1] * part.shape[2] * part.shape[3] * cap

        def gate_up(j, unused):
            both = jnp.dot(
                rows[k].reshape(flat_rows, width), wgu[j], preferred_element_type=jnp.float32
            )
            gate = both[:, :half]
            hidden[:, pl.ds(pl.multiple_of(j * half, half), half)] = (
                gate / (1.0 + jnp.exp(-gate)) * both[:, half:]
            ).astype(jnp.bfloat16)
            return unused

        lax.fori_loop(0, tiles, gate_up, 0)

        def down(j, unused):
            lanes = pl.ds(pl.multiple_of(j * strip, strip), strip)
            value = jnp.dot(hidden[...], wd[:, lanes], preferred_element_type=jnp.float32)
            part[k, :, :, :, :, lanes] = value.astype(jnp.bfloat16).reshape(part.shape[1:5] + (strip,))
            send_p(k, j).start()
            return unused

        lax.fori_loop(0, width // strip, down, 0)

    def send_p(k, j):
        lanes = pl.ds(pl.multiple_of(j * strip, strip), strip)
        return remote(
            part.at[k, 1 - c, :, :, :, lanes], got.at[k, :, :, :, lanes], p_send.at[k, j], p_recv.at[k, j], mate
        )

    def cross_p(k, n):
        return remote(sum_out.at[k, n], sum_in.at[k, n], s_send.at[k, n], s_recv.at[k, n], across)

    def send_back(d):
        return remote(back_out.at[d], back_in.at[d], b_send.at[d], b_recv.at[d], {"ep": xor(me, d, ep)})

    def own_rows(ds):
        for d in ds:
            dispatch(d).wait_recv()
            if d not in direct:
                forward_x(d).start()
            forward_c(d).start()

    def cross_rows(ds):
        for d in ds:
            forward_x(d).wait_recv()
            forward_xc(d).start()

    def first_sum(k):
        for j in range(width // strip):
            send_p(k, j).wait_recv()

        def add(n, unused):
            total = part[k, c, n, 1 - x].astype(jnp.float32) + got[k, n, 1 - x].astype(jnp.float32)
            sum_out[k, n] = total.astype(jnp.bfloat16)
            cross_p(k, n).start()
            return unused

        lax.fori_loop(0, per, add, 0)

    def last_sum(k):
        for n, d in enumerate(groups[k]):
            cross_p(k, n).wait_recv()
            total = (
                part[k, c, n, x].astype(jnp.float32)
                + got[k, n, x].astype(jnp.float32)
                + sum_in[k, n].astype(jnp.float32)
            )
            back_out[d] = total.astype(jnp.bfloat16)
            if d > 0:
                send_back(d).start()

    expert_steps = (unit, 3 * unit, 4 * unit, 6 * unit)

    def step(i, unused):
        @pl.when(i == 2 * unit)
        def _():
            own_rows(groups[2])

        @pl.when(i == 4 * unit)
        def _():
            own_rows(groups[3])

        @pl.when(i == 0)
        def _():
            tile(k_ref, v_ref, bias_ref, place < key_ids)

        @pl.when((i > 0) & (i <= me))
        def _():
            source = me - i

            @pl.when(i % 2 == 1)
            def _():
                wait_kv(source)

            tile(kbuf.at[source], vbuf.at[source], bbuf.at[source], None)

        @pl.when((i % 2 == 0) & (i + 2 <= me))
        def _():
            source = me - i - 2
            wait_kv(source)
            for copy in passed_kv(source, pair, kv_psend):
                copy.start()

            @pl.when(up < upper - 1)
            def _():
                for copy in passed_kv(source, me + 2, kv_zsend):
                    copy.start()

        @pl.when(i == me)
        def _():
            wo_copy.wait()
            project()
            send_a().start()

        @pl.when(i == me + 1)
        def _():
            send_a().wait_recv()
            sum_out_a[...] = (
                part_a[c, 1 - x].astype(jnp.float32) + got_a[1 - x].astype(jnp.float32)
            ).astype(jnp.bfloat16)
            cross_a().start()

        @pl.when(i == expert_steps[0])
        def _():
            for copy in weight_copies():
                copy.wait()

        @pl.when(i == 0)
        def _():
            own_rows(groups[0][1:])

        @pl.when(i == unit)
        def _():
            for d in groups[3]:
                dispatch(d).start()
            cross_rows(groups[0])

        @pl.when(i == 3 * unit)
        def _():
            cross_rows(groups[2])

        @pl.when(i == 4 * unit)
        def _():
            cross_rows(groups[1][per // 2 :])

        @pl.when(i == 6 * unit)
        def _():
            cross_rows(groups[3])

        @pl.when((i == expert_steps[0]) | (i == expert_steps[1]) | (i == expert_steps[2]) | (i == expert_steps[3]))
        def _():
            k = 0
            for later, more in zip(expert_steps[1:], (2, -1, 2)):
                k = k + jnp.where(i >= later, more, 0)

            def landed(n, unused):
                ref = rows.at[k, c, n, x]
                for way in range(2):
                    remote(ref, ref, c_send.at[k * per + n, way], c_recv.at[k * per + n, way], mate).wait_recv()
                return unused

            lax.fori_loop(0, per, landed, 0)
            experts(k)

        @pl.when(i == unit)
        def _():
            own_rows(groups[1][: per // 2])

        @pl.when(i == 2 * unit)
        def _():
            own_rows(groups[1][per // 2 :])
            cross_rows(groups[1][: per // 2])

        @pl.when(i == 3 * unit)
        def _():
            first_sum(2)

        @pl.when(i == 5 * unit)
        def _():
            first_sum(0)
            last_sum(2)

        @pl.when(i == 6 * unit)
        def _():
            first_sum(3)
            first_sum(1)

        @pl.when(i == 7 * unit)
        def _():
            last_sum(0)
            last_sum(3)

        @pl.when(i == 8 * unit)
        def _():
            last_sum(1)

        return unused

    lax.fori_loop(0, 8 * unit + 1, step, 0)
    cross_a().wait_recv()
    out_a_ref[...] = (
        part_a[c, x].astype(jnp.float32) + got_a[x].astype(jnp.float32) + sum_in_a[...].astype(jnp.float32)
    ).astype(jnp.bfloat16)

    back_in[0] = back_out[0]

    def returned(d, unused):
        remote(back_out.at[d], back_in.at[d], b_send.at[d], b_recv.at[d], mate).wait_recv()
        return unused

    lax.fori_loop(1, ep, returned, 0)
    for d in range(ep):
        picks = routes_ref[...] == xor(me, d, ep)
        weight = jnp.sum(jnp.where(picks, mix_ref[...], 0.0), axis=0, keepdims=True)
        share = hit[d].astype(jnp.float32) * weight
        high = share.astype(bf16)
        share_high[d] = high
        share_low[d] = (share - high.astype(jnp.float32)).astype(bf16)
    over_rows = (((0,), (0,)), ((), ()))
    for lane in range(0, width, strip):
        piece = back_in[:, :, lane : lane + strip].reshape(ep * cap, strip)
        total = lax.dot_general(
            share_high[...].reshape(ep * cap, tok), piece, over_rows, preferred_element_type=jnp.float32
        ) + lax.dot_general(
            share_low[...].reshape(ep * cap, tok), piece, over_rows, preferred_element_type=jnp.float32
        )
        out_b_ref[:, lane : lane + strip] = total.astype(bf16)

    @pl.when(odd == 0)
    def _():
        for copy in own_kv(pair, kv_psend.at[me]):
            copy.wait_send()

    @pl.when(up < upper - 1)
    def _():
        for copy in own_kv(me + 2, kv_zsend.at[me]):
            copy.wait_send()

    def left_pair(step, unused):
        source = me - 2 * step
        for copy in passed_kv(source, pair, kv_psend):
            copy.wait_send()

        @pl.when(up < upper - 1)
        def _():
            for copy in passed_kv(source, me + 2, kv_zsend):
                copy.wait_send()

        return unused

    lax.fori_loop(1, up + 1, left_pair, 0)

    for d in range(ep):
        if d > 0:
            dispatch(d).wait_send()
            send_back(d).wait_send()
        forward_x(d).wait_send()
        forward_c(d).wait_send()
        forward_xc(d).wait_send()

    def left_sums(k, unused):
        for j in range(width // strip):
            send_p(k, j).wait_send()

        def left_cross(n, unused):
            cross_p(k, n).wait_send()
            return unused

        lax.fori_loop(0, per, left_cross, 0)
        return unused

    lax.fori_loop(0, chunks, left_sums, 0)
    send_a().wait_send()
    cross_a().wait_send()


def body(
    query_rows,
    key_rows,
    value_rows,
    key_bias,
    head_offset,
    out_weight,
    expert_input,
    expert_gain,
    routes,
    route_weight,
    gate_weight,
    up_weight,
    down_weight,
):
    ep, tp = lax.axis_size("ep"), lax.axis_size("tp")
    block = key_rows.shape[0]
    kv_local = key_rows.shape[1] // HD
    heads = query_rows.shape[1] // HD
    tok, width = expert_input.shape
    top = routes.shape[1]
    hidden_width = gate_weight.shape[2]
    cap = max(2, 3 * tok * top // (2 * ep))
    cap = -(-cap // 16) * 16
    chunks = 4
    per = ep // chunks
    across = tp // CORES
    half = 128
    tiles = hidden_width // half
    vmem = pl.BlockSpec(memory_space=pltpu.VMEM)
    hbm = pl.BlockSpec(memory_space=pl.ANY)
    bf16, f32, dma = jnp.bfloat16, jnp.float32, pltpu.SemaphoreType.DMA
    own_a = block // tp
    wide = kv_local * HD
    return pl.pallas_call(
        functools.partial(step_kernel, ep=ep, chunks=chunks, group_size=heads // kv_local, kv_local=kv_local),
        out_shape=(
            jax.ShapeDtypeStruct((own_a, width), bf16),
            jax.ShapeDtypeStruct((tok, width), bf16),
        ),
        in_specs=[vmem] * 4 + [pl.BlockSpec(memory_space=pltpu.SMEM)] + [vmem] * 4 + [hbm] * 4,
        out_specs=(vmem, vmem),
        scratch_shapes=[
            pltpu.VMEM((heads, block, wide), bf16),
            pltpu.VMEM((ep, block, wide), bf16),
            pltpu.VMEM((ep, block, wide), bf16),
            pltpu.VMEM((ep, kv_local, block), bf16),
            pltpu.VMEM((heads, block, wide), f32),
            pltpu.VMEM((heads, block, 1), f32),
            pltpu.VMEM((block, heads * HD), bf16),
            pltpu.VMEM((block, block), bf16),
            pltpu.VMEM((ep, cap, tok), bf16),
            pltpu.VMEM((ep, cap, tok), bf16),
            pltpu.VMEM((ep, cap, tok), bf16),
            pltpu.VMEM((ep, cap, width), bf16),
            pltpu.VMEM((chunks, CORES, per, across, cap, width), bf16),
            pltpu.VMEM((CORES * per * across * cap, hidden_width), bf16),
            pltpu.VMEM((chunks, CORES, per, across, cap, width), bf16),
            pltpu.VMEM((chunks, per, across, cap, width), bf16),
            pltpu.VMEM((chunks, per, cap, width), bf16),
            pltpu.VMEM((chunks, per, cap, width), bf16),
            pltpu.VMEM((ep, cap, width), bf16),
            pltpu.VMEM((ep, cap, width), bf16),
            pltpu.VMEM((CORES, across, own_a, width), bf16),
            pltpu.VMEM((across, own_a, width), bf16),
            pltpu.VMEM((own_a, width), bf16),
            pltpu.VMEM((own_a, width), bf16),
            pltpu.VMEM((tiles, width, 2 * half), bf16),
            pltpu.VMEM((hidden_width, width), bf16),
            pltpu.VMEM((heads * HD, width), bf16),
            dma((2 * tiles + 2,)),
            dma((ep, 3)),
            dma((ep, 3)),
            dma((ep, 3)),
            dma((ep,)), dma((ep,)), dma((ep,)), dma((ep,)), dma((ep, 2)), dma((ep, 2)),
            dma((chunks, width // 512)), dma((chunks, width // 512)), dma((chunks, per)), dma((chunks, per)), dma((ep,)), dma((ep,)),
            dma((2,)), dma((2,)),
        ],
        compiler_params=pltpu.CompilerParams(
            collective_id=0, has_side_effects=True, vmem_limit_bytes=60 * 1024 * 1024
        ),
        name="step",
    )(
        query_rows, key_rows, value_rows, key_bias.T, head_offset, expert_input, expert_gain[None, :],
        routes.T, route_weight.T, out_weight, gate_weight, up_weight, down_weight,
    )


def solution(mesh):
    return jax.shard_map(
        body,
        mesh=mesh,
        in_specs=(
            P("ep", "tp"),
            P("ep", "tp"),
            P("ep", "tp"),
            P("ep", "tp"),
            P("tp"),
            P("tp", None),
            P(("ep", "tp"), None),
            P(),
            P(("ep", "tp"), None),
            P(("ep", "tp"), None),
            P("ep", None, "tp"),
            P("ep", None, "tp"),
            P("ep", "tp", None),
        ),
        out_specs=(P(("ep", "tp"), None), P(("ep", "tp"), None)),
        check_vma=False,
    )
```

```python
import functools
import math

import jax
import jax.numpy as jnp
from jax import lax
from jax.experimental import pallas as pl
from jax.experimental.pallas import tpu as pltpu
from jax.sharding import PartitionSpec as P

HD = 64
EPSILON = 1e-06
LOG2E = 1.4426950408889634
MESH = pl.DeviceIdType.MESH
CORES = 2


def xor(a, b, size):
    total, bit = 0, 1
    while bit < size:
        total = total + bit * ((a // bit + b // bit) % 2)
        bit *= 2
    return total


def step_kernel(
    q_ref, k_ref, v_ref, bias_ref, offset_ref, x_ref, gain_ref, routes_ref, mix_ref,
    wo_hbm, wg_hbm, wu_hbm, wd_hbm,
    out_a_ref, out_b_ref,
    qw, kbuf, vbuf, bbuf, acc, carry, heads_out, tri,
    hit, share_high, share_low, outgoing, rows, hidden, part, got, sum_out, sum_in, back_out, back_in,
    part_a, got_a, sum_out_a, sum_in_a,
    wgu, wd, wo,
    w_sem, kv_zsend, kv_psend, kv_recv,
    d_send, d_recv, x_send, x_recv, c_send, c_recv, p_send, p_recv, s_send, s_recv, b_send, b_recv,
    a_send, a_recv,
    *, ep, chunks, group_size, kv_local,
):
    me = lax.axis_index("ep")
    t = lax.axis_index("tp")
    c = t % CORES
    x = t // CORES
    mate = {"tp": CORES * x + 1 - c}
    across = {"tp": CORES * (1 - x) + c}
    per = ep // chunks
    unit = per // 2
    cap = outgoing.shape[1]
    width = outgoing.shape[2]
    block = k_ref.shape[0]
    heads = kv_local * group_size
    up = me // 2
    upper = ep // 2
    odd = me % 2
    pair = me + 1 - 2 * odd

    def remote(src, dst, send, recv, device):
        return pltpu.make_async_remote_copy(
            src_ref=src, dst_ref=dst, send_sem=send, recv_sem=recv, device_id=device, device_id_type=MESH
        )

    tiles = wgu.shape[0]
    half = wgu.shape[2] // 2

    def weight_copies():
        copies = []
        for tile in range(tiles):
            lanes = slice(tile * half, (tile + 1) * half)
            copies.append(pltpu.make_async_copy(wg_hbm.at[0, :, lanes], wgu.at[tile, :, 0:half], w_sem.at[2 * tile]))
            copies.append(
                pltpu.make_async_copy(wu_hbm.at[0, :, lanes], wgu.at[tile, :, half : 2 * half], w_sem.at[2 * tile + 1])
            )
        copies.append(pltpu.make_async_copy(wd_hbm.at[0], wd, w_sem.at[2 * tiles]))
        return copies

    wo_copy = pltpu.make_async_copy(wo_hbm, wo, w_sem.at[2 * tiles + 1])
    wo_copy.start()
    for copy in weight_copies():
        copy.start()

    direct = range(1, per + per // 2)
    barrier = pltpu.get_barrier_semaphore()

    def greet(step, unused):
        pl.semaphore_signal(barrier, inc=1, device_id={"ep": (me + step) % ep}, device_id_type=MESH)
        return unused

    lax.fori_loop(1, ep, greet, 0)
    pl.semaphore_signal(barrier, inc=1, device_id=mate, device_id_type=MESH)
    pl.semaphore_signal(barrier, inc=1, device_id=across, device_id_type=MESH)
    for d in direct:
        device = {"ep": xor(me, d, ep), "tp": CORES * (1 - x) + c}
        pl.semaphore_signal(barrier, inc=1, device_id=device, device_id_type=MESH)

    values = x_ref[...].astype(jnp.float32)
    scale = lax.rsqrt(jnp.mean(values * values, axis=-1, keepdims=True) + EPSILON)
    normed = (values * scale * gain_ref[...]).astype(jnp.bfloat16)
    tok = normed.shape[0]
    bf16 = jnp.bfloat16
    expert_ids = xor(lax.broadcasted_iota(jnp.int32, (ep, tok), 0), me, ep)
    named = jnp.where((routes_ref[0:1, :] == expert_ids) | (routes_ref[1:2, :] == expert_ids), 1.0, 0.0)
    earlier = lax.broadcasted_iota(jnp.int32, (tok, tok), 0) < lax.broadcasted_iota(jnp.int32, (tok, tok), 1)
    rank = jnp.dot(named.astype(bf16), jnp.where(earlier, 1.0, 0.0).astype(bf16), preferred_element_type=jnp.float32)
    rank = jnp.where(named > 0.0, rank, -1.0)
    spots = lax.broadcasted_iota(jnp.int32, (cap, tok), 0).astype(jnp.float32)
    for d in range(ep):
        hit[d] = jnp.where(rank[d : d + 1, :] == spots, 1.0, 0.0).astype(bf16)
    strip = 512
    for lane in range(0, width, strip):
        picked = jnp.dot(hit[...].reshape(ep * cap, tok), normed[:, lane : lane + strip], preferred_element_type=jnp.float32)
        outgoing[:, :, lane : lane + strip] = picked.astype(jnp.bfloat16).reshape(ep, cap, strip)
    rows[0, c, 0, x] = outgoing[0]

    lane_ids = lax.broadcasted_iota(jnp.int32, (kv_local * HD, kv_local * HD), 1)
    row_ids = lax.broadcasted_iota(jnp.int32, (kv_local * HD, kv_local * HD), 0)
    wide = kv_local * HD
    for head in range(heads):
        kv = head // group_size
        first = head * HD // wide * wide
        shift = head * HD - first - kv * HD
        move = jnp.where((row_ids == lane_ids + shift) & (lane_ids // HD == kv), 1.0, 0.0).astype(jnp.bfloat16)
        qw[head] = jnp.dot(
            q_ref[:, first : first + wide], move, preferred_element_type=jnp.float32
        ).astype(jnp.bfloat16)
    key_ids = lax.broadcasted_iota(jnp.int32, (block, block), 0)
    place = lax.broadcasted_iota(jnp.int32, (block, block), 1)
    tri[...] = jnp.where(key_ids > place, 1.0, 0.0).astype(jnp.bfloat16)
    acc[...] = jnp.zeros_like(acc)
    carry[...] = jnp.zeros_like(carry)

    pl.semaphore_wait(barrier, ep + 1 + len(direct))

    def own_kv(target, sems):
        return [
            remote(k_ref, kbuf.at[me], sems.at[0], kv_recv.at[me, 0], {"ep": target}),
            remote(v_ref, vbuf.at[me], sems.at[1], kv_recv.at[me, 1], {"ep": target}),
            remote(bias_ref, bbuf.at[me], sems.at[2], kv_recv.at[me, 2], {"ep": target}),
        ]

    def passed_kv(source, target, sems):
        return [
            remote(ref.at[source], ref.at[source], sems.at[source, i], kv_recv.at[source, i], {"ep": target})
            for i, ref in enumerate((kbuf, vbuf, bbuf))
        ]

    @pl.when(odd == 0)
    def _():
        for copy in own_kv(pair, kv_psend.at[me]):
            copy.start()

    @pl.when(up < upper - 1)
    def _():
        for copy in own_kv(me + 2, kv_zsend.at[me]):
            copy.start()

    groups = [range(k * per, (k + 1) * per) for k in range(chunks)]

    def slot_of(d):
        return rows.at[d // per, c, d % per, x]

    def dispatch(d):
        return remote(outgoing.at[d], slot_of(d), d_send.at[d], d_recv.at[d], {"ep": xor(me, d, ep)})

    def dispatch_across(d):
        device = {"ep": xor(me, d, ep), "tp": CORES * (1 - x) + c}
        return remote(outgoing.at[d], slot_of(d), x_send.at[d], x_recv.at[d], device)

    def forward_x(d):
        return remote(slot_of(d), slot_of(d), x_send.at[d], x_recv.at[d], across)

    def forward_c(d):
        return remote(slot_of(d), slot_of(d), c_send.at[d, 0], c_recv.at[d, 0], mate)

    def forward_xc(d):
        ref = rows.at[d // per, c, d % per, 1 - x]
        return remote(ref, ref, c_send.at[d, 1], c_recv.at[d, 1], mate)

    forward_x(0).start()
    forward_c(0).start()
    for d in list(groups[0][1:]) + [d for pair_of in zip(groups[2], groups[1]) for d in pair_of]:
        dispatch(d).start()
        if d in direct:
            dispatch_across(d).start()

    def tile(keys, vals, biases, keep):
        for head in range(heads):
            kv = head // group_size
            raw = lax.dot_general(
                qw[head], keys[...], (((1,), (1,)), ((), ())), preferred_element_type=jnp.float32
            )
            row = (biases[kv : kv + 1, :].astype(jnp.float32) + offset_ref[head]) * LOG2E
            scores = raw * (LOG2E / math.sqrt(HD)) + row
            soft = jnp.log2(1.0 + jnp.exp2(-jnp.abs(scores)))
            leave = jnp.maximum(scores, 0.0) + soft
            log_take = jnp.minimum(scores, 0.0) - soft
            if keep is not None:
                leave = jnp.where(keep, leave, 0.0)
            high = leave.astype(jnp.bfloat16)
            after = jnp.dot(high, tri[...], preferred_element_type=jnp.float32)
            before = carry[head]
            weights = jnp.exp2(log_take - after - before)
            if keep is not None:
                weights = jnp.where(keep, weights, 0.0)
            acc[head] += jnp.dot(weights.astype(jnp.bfloat16), vals[...], preferred_element_type=jnp.float32)
            carry[head] = before + after[:, :1] + leave[:, :1]

    def wait_kv(source):
        for i, ref in enumerate((kbuf, vbuf, bbuf)):
            remote(ref.at[source], ref.at[source], kv_psend.at[source, i], kv_recv.at[source, i], mate).wait_recv()

    def project():
        lanes = slice(0, 0)
        pieces = []
        for head in range(heads):
            kv = head // group_size
            lanes = slice(kv * HD, (kv + 1) * HD)
            pieces.append(acc[head, :, lanes].astype(jnp.bfloat16))
        for head in range(heads):
            heads_out[:, head * HD : (head + 1) * HD] = pieces[head]
        own = part_a.shape[2]
        for lane in range(0, width, strip):
            value = jnp.dot(heads_out[...], wo[:, lane : lane + strip], preferred_element_type=jnp.float32)
            value = value.astype(jnp.bfloat16).reshape(2, CORES, own, strip)
            for xs in range(2):
                for cs in range(CORES):
                    part_a[cs, xs, :, lane : lane + strip] = value[xs, cs]

    def send_a():
        return remote(part_a.at[1 - c], got_a, a_send.at[0], a_recv.at[0], mate)

    def cross_a():
        return remote(sum_out_a, sum_in_a, a_send.at[1], a_recv.at[1], across)

    def experts(k):
        flat_rows = part.shape[1] * part.shape[2] * part.shape[3] * cap

        def gate_up(j, unused):
            both = jnp.dot(
                rows[k].reshape(flat_rows, width), wgu[j], preferred_element_type=jnp.float32
            )
            gate = both[:, :half]
            hidden[:, pl.ds(pl.multiple_of(j * half, half), half)] = (
                gate / (1.0 + jnp.exp(-gate)) * both[:, half:]
            ).astype(jnp.bfloat16)
            return unused

        lax.fori_loop(0, tiles, gate_up, 0, unroll=True)

        def down(j, unused):
            lanes = pl.ds(pl.multiple_of(j * strip, strip), strip)
            value = jnp.dot(hidden[...], wd[:, lanes], preferred_element_type=jnp.float32)
            part[k, :, :, :, :, lanes] = value.astype(jnp.bfloat16).reshape(part.shape[1:5] + (strip,))
            send_p(k, j).start()
            return unused

        lax.fori_loop(0, width // strip, down, 0, unroll=True)

    def send_p(k, j):
        lanes = pl.ds(pl.multiple_of(j * strip, strip), strip)
        return remote(
            part.at[k, 1 - c, :, :, :, lanes], got.at[k, :, :, :, lanes], p_send.at[k, j], p_recv.at[k, j], mate
        )

    def cross_p(k, n):
        return remote(sum_out.at[k, n], sum_in.at[k, n], s_send.at[k, n], s_recv.at[k, n], across)

    def send_back(d):
        return remote(back_out.at[d], back_in.at[d], b_send.at[d], b_recv.at[d], {"ep": xor(me, d, ep)})

    def own_rows(ds):
        for d in ds:
            dispatch(d).wait_recv()
            if d not in direct:
                forward_x(d).start()
            forward_c(d).start()

    def cross_rows(ds):
        for d in ds:
            forward_x(d).wait_recv()
            forward_xc(d).start()

    def first_sum(k):
        for j in range(width // strip):
            send_p(k, j).wait_recv()

        def add(n, unused):
            total = part[k, c, n, 1 - x].astype(jnp.float32) + got[k, n, 1 - x].astype(jnp.float32)
            sum_out[k, n] = total.astype(jnp.bfloat16)
            cross_p(k, n).start()
            return unused

        lax.fori_loop(0, per, add, 0)

    def last_sum(k):
        for n, d in enumerate(groups[k]):
            cross_p(k, n).wait_recv()
            total = (
                part[k, c, n, x].astype(jnp.float32)
                + got[k, n, x].astype(jnp.float32)
                + sum_in[k, n].astype(jnp.float32)
            )
            back_out[d] = total.astype(jnp.bfloat16)
            if d > 0:
                send_back(d).start()

    expert_steps = (unit, 3 * unit, 4 * unit, 5 * unit)

    def tile_at(i):
        return i

    def hook(j):
        source = me - 2 * j
        wait_kv(source)
        for copy in passed_kv(source, pair, kv_psend):
            copy.start()

        @pl.when(up < upper - 1)
        def _():
            for copy in passed_kv(source, me + 2, kv_zsend):
                copy.start()

    def step(i, unused):
        @pl.when(i == 2 * unit)
        def _():
            own_rows(groups[2])

        @pl.when(i == 4 * unit)
        def _():
            own_rows(groups[3])
            first_sum(2)

        @pl.when(i == 0)
        def _():
            tile(k_ref, v_ref, bias_ref, place < key_ids)

        @pl.when(i == unit)
        def _():
            for d in groups[3]:
                dispatch(d).start()

        def earlier_tile(n, unused):
            source = me - n

            @pl.when(n % 2 == 1)
            def _():
                wait_kv(source)

            tile(kbuf.at[source], vbuf.at[source], bbuf.at[source], None)
            return unused

        start, stop = tile_at(i), tile_at(i + 1)
        lax.fori_loop(jnp.where(i == 0, 1, start), jnp.minimum(stop, me + 1), earlier_tile, 0)

        @pl.when((i % 2 == 0) & (i // 2 + 1 <= up))
        def _():
            hook(i // 2 + 1)

        @pl.when((start <= me) & (me < stop))
        def _():
            wo_copy.wait()
            project()
            send_a().start()

        @pl.when((i > 0) & (tile_at(i - 1) <= me) & (me < start))
        def _():
            send_a().wait_recv()
            sum_out_a[...] = (
                part_a[c, 1 - x].astype(jnp.float32) + got_a[1 - x].astype(jnp.float32)
            ).astype(jnp.bfloat16)
            cross_a().start()

        @pl.when(i == expert_steps[0])
        def _():
            for copy in weight_copies():
                copy.wait()

        @pl.when(i == 0)
        def _():
            own_rows(groups[0][1:])

        @pl.when(i == unit)
        def _():
            cross_rows(groups[0])

        @pl.when(i == 3 * unit)
        def _():
            cross_rows(groups[2])

        @pl.when(i == 4 * unit)
        def _():
            cross_rows(groups[1][per // 2 :])

        @pl.when(i == 5 * unit)
        def _():
            cross_rows(groups[3])

        @pl.when((i == expert_steps[0]) | (i == expert_steps[1]) | (i == expert_steps[2]) | (i == expert_steps[3]))
        def _():
            k = 0
            for later, more in zip(expert_steps[1:], (2, -1, 2)):
                k = k + jnp.where(i >= later, more, 0)

            def landed(n, unused):
                ref = rows.at[k, c, n, x]
                for way in range(2):
                    remote(ref, ref, c_send.at[k * per + n, way], c_recv.at[k * per + n, way], mate).wait_recv()
                return unused

            lax.fori_loop(0, per, landed, 0)
            experts(k)

        @pl.when(i == unit)
        def _():
            own_rows(groups[1][: per // 2])

        @pl.when(i == 2 * unit)
        def _():
            own_rows(groups[1][per // 2 :])
            cross_rows(groups[1][: per // 2])

        @pl.when(i == 5 * unit)
        def _():
            first_sum(3)
            last_sum(2)

        @pl.when(i == 6 * unit)
        def _():
            first_sum(1)
            first_sum(0)
            last_sum(3)

        @pl.when(i == 7 * unit)
        def _():
            last_sum(1)

        @pl.when(i == 8 * unit)
        def _():
            last_sum(0)

        return unused

    lax.fori_loop(0, 8 * unit + 1, step, 0)
    cross_a().wait_recv()
    out_a_ref[...] = (
        part_a[c, x].astype(jnp.float32) + got_a[x].astype(jnp.float32) + sum_in_a[...].astype(jnp.float32)
    ).astype(jnp.bfloat16)

    back_in[0] = back_out[0]

    def returned(d, unused):
        remote(back_out.at[d], back_in.at[d], b_send.at[d], b_recv.at[d], mate).wait_recv()
        return unused

    lax.fori_loop(1, ep, returned, 0)
    for d in range(ep):
        picks = routes_ref[...] == xor(me, d, ep)
        weight = jnp.sum(jnp.where(picks, mix_ref[...], 0.0), axis=0, keepdims=True)
        share = hit[d].astype(jnp.float32) * weight
        high = share.astype(bf16)
        share_high[d] = high
        share_low[d] = (share - high.astype(jnp.float32)).astype(bf16)
    over_rows = (((0,), (0,)), ((), ()))
    for lane in range(0, width, strip):
        piece = back_in[:, :, lane : lane + strip].reshape(ep * cap, strip)
        total = lax.dot_general(
            share_high[...].reshape(ep * cap, tok), piece, over_rows, preferred_element_type=jnp.float32
        ) + lax.dot_general(
            share_low[...].reshape(ep * cap, tok), piece, over_rows, preferred_element_type=jnp.float32
        )
        out_b_ref[:, lane : lane + strip] = total.astype(bf16)

    @pl.when(odd == 0)
    def _():
        for copy in own_kv(pair, kv_psend.at[me]):
            copy.wait_send()

    @pl.when(up < upper - 1)
    def _():
        for copy in own_kv(me + 2, kv_zsend.at[me]):
            copy.wait_send()

    def left_pair(step, unused):
        source = me - 2 * step
        for copy in passed_kv(source, pair, kv_psend):
            copy.wait_send()

        @pl.when(up < upper - 1)
        def _():
            for copy in passed_kv(source, me + 2, kv_zsend):
                copy.wait_send()

        return unused

    lax.fori_loop(1, up + 1, left_pair, 0)

    for d in range(ep):
        if d > 0:
            dispatch(d).wait_send()
            send_back(d).wait_send()
        forward_x(d).wait_send()
        forward_c(d).wait_send()
        forward_xc(d).wait_send()

    def left_sums(k, unused):
        for j in range(width // strip):
            send_p(k, j).wait_send()

        def left_cross(n, unused):
            cross_p(k, n).wait_send()
            return unused

        lax.fori_loop(0, per, left_cross, 0)
        return unused

    lax.fori_loop(0, chunks, left_sums, 0)
    send_a().wait_send()
    cross_a().wait_send()


def body(
    query_rows,
    key_rows,
    value_rows,
    key_bias,
    head_offset,
    out_weight,
    expert_input,
    expert_gain,
    routes,
    route_weight,
    gate_weight,
    up_weight,
    down_weight,
):
    ep, tp = lax.axis_size("ep"), lax.axis_size("tp")
    block = key_rows.shape[0]
    kv_local = key_rows.shape[1] // HD
    heads = query_rows.shape[1] // HD
    tok, width = expert_input.shape
    top = routes.shape[1]
    hidden_width = gate_weight.shape[2]
    cap = max(2, 3 * tok * top // (2 * ep))
    cap = -(-cap // 16) * 16
    chunks = 4
    per = ep // chunks
    across = tp // CORES
    half = 128
    tiles = hidden_width // half
    vmem = pl.BlockSpec(memory_space=pltpu.VMEM)
    hbm = pl.BlockSpec(memory_space=pl.ANY)
    bf16, f32, dma = jnp.bfloat16, jnp.float32, pltpu.SemaphoreType.DMA
    own_a = block // tp
    wide = kv_local * HD
    return pl.pallas_call(
        functools.partial(step_kernel, ep=ep, chunks=chunks, group_size=heads // kv_local, kv_local=kv_local),
        out_shape=(
            jax.ShapeDtypeStruct((own_a, width), bf16),
            jax.ShapeDtypeStruct((tok, width), bf16),
        ),
        in_specs=[vmem] * 4 + [pl.BlockSpec(memory_space=pltpu.SMEM)] + [vmem] * 4 + [hbm] * 4,
        out_specs=(vmem, vmem),
        scratch_shapes=[
            pltpu.VMEM((heads, block, wide), bf16),
            pltpu.VMEM((ep, block, wide), bf16),
            pltpu.VMEM((ep, block, wide), bf16),
            pltpu.VMEM((ep, kv_local, block), bf16),
            pltpu.VMEM((heads, block, wide), f32),
            pltpu.VMEM((heads, block, 1), f32),
            pltpu.VMEM((block, heads * HD), bf16),
            pltpu.VMEM((block, block), bf16),
            pltpu.VMEM((ep, cap, tok), bf16),
            pltpu.VMEM((ep, cap, tok), bf16),
            pltpu.VMEM((ep, cap, tok), bf16),
            pltpu.VMEM((ep, cap, width), bf16),
            pltpu.VMEM((chunks, CORES, per, across, cap, width), bf16),
            pltpu.VMEM((CORES * per * across * cap, hidden_width), bf16),
            pltpu.VMEM((chunks, CORES, per, across, cap, width), bf16),
            pltpu.VMEM((chunks, per, across, cap, width), bf16),
            pltpu.VMEM((chunks, per, cap, width), bf16),
            pltpu.VMEM((chunks, per, cap, width), bf16),
            pltpu.VMEM((ep, cap, width), bf16),
            pltpu.VMEM((ep, cap, width), bf16),
            pltpu.VMEM((CORES, across, own_a, width), bf16),
            pltpu.VMEM((across, own_a, width), bf16),
            pltpu.VMEM((own_a, width), bf16),
            pltpu.VMEM((own_a, width), bf16),
            pltpu.VMEM((tiles, width, 2 * half), bf16),
            pltpu.VMEM((hidden_width, width), bf16),
            pltpu.VMEM((heads * HD, width), bf16),
            dma((2 * tiles + 2,)),
            dma((ep, 3)),
            dma((ep, 3)),
            dma((ep, 3)),
            dma((ep,)), dma((ep,)), dma((ep,)), dma((ep,)), dma((ep, 2)), dma((ep, 2)),
            dma((chunks, width // 512)), dma((chunks, width // 512)), dma((chunks, per)), dma((chunks, per)), dma((ep,)), dma((ep,)),
            dma((2,)), dma((2,)),
        ],
        compiler_params=pltpu.CompilerParams(
            collective_id=0, has_side_effects=True, vmem_limit_bytes=60 * 1024 * 1024
        ),
        name="step",
    )(
        query_rows, key_rows, value_rows, key_bias.T, head_offset, expert_input, expert_gain[None, :],
        routes.T, route_weight.T, out_weight, gate_weight, up_weight, down_weight,
    )


def solution(mesh):
    return jax.shard_map(
        body,
        mesh=mesh,
        in_specs=(
            P("ep", "tp"),
            P("ep", "tp"),
            P("ep", "tp"),
            P("ep", "tp"),
            P("tp"),
            P("tp", None),
            P(("ep", "tp"), None),
            P(),
            P(("ep", "tp"), None),
            P(("ep", "tp"), None),
            P("ep", None, "tp"),
            P("ep", None, "tp"),
            P("ep", "tp", None),
        ),
        out_specs=(P(("ep", "tp"), None), P(("ep", "tp"), None)),
        check_vma=False,
    )
```
